32 devices in a mesh: grp: 2 (over x), fs: 4 (over z), tp: 4 (over y, core).
Axes of the slice: x: 2, y: 2, z: 4, core: 2. Of those that a mesh axis runs over, the one named last changes fastest.
Arguments:
- tokens: bfloat16 [2048, 2048], P(('grp', 'fs'), 'tp'), parts along dimension 0, may hold values from -12 to 12
- gain_first: float32 [2048], P('tp'), may hold values from 0.1 to 1.9
- gate_first: float32 [2048, 5632], P('fs', 'tp'), may hold values from -0.125 to 0.125
- gate_scale_first: float32 [5632], P('tp'), may hold values from 0.5 to 2
- up_first: float32 [2048, 5632], P('fs', 'tp'), may hold values from -0.125 to 0.125
- up_scale_first: float32 [5632], P('tp'), may hold values from 0.5 to 2
- down_first: float32 [5632, 2048], P('tp', 'fs'), may hold values from -0.078125 to 0.078125
- down_scale_first: float32 [2048], P('tp'), may hold values from 0.5 to 2
- gain_second: float32 [2048], P('tp'), may hold values from 0.1 to 1.9
- gate_second: float32 [2048, 5632], P('fs', 'tp'), may hold values from -0.125 to 0.125
- gate_scale_second: float32 [5632], P('tp'), may hold values from 0.5 to 2
- up_second: float32 [2048, 5632], P('fs', 'tp'), may hold values from -0.125 to 0.125
- up_scale_second: float32 [5632], P('tp'), may hold values from 0.5 to 2
- down_second: float32 [5632, 2048], P('tp', 'fs'), may hold values from -0.078125 to 0.078125
- down_scale_second: float32 [2048], P('tp'), may hold values from 0.5 to 2
Outputs:
- stream_out: bfloat16 [2048, 2048], P(('grp', 'fs'), 'tp'), parts along dimension 0
The draws below stay inside these ranges and needn't reach their ends.
There are 2 independent parts, one for each index of `grp`. The reference program is written for one: setup_inputs(seed, part) draws one part's arguments, and reference() takes and returns one part's arrays. A program takes and returns all parts, laid end to end along the dimension named above; an argument that names none is the same for every part. Nothing has to cross between parts.
All inputs are finite; a program needn't handle non-finite values.
Results may differ from the reference program's by a relative error of at most 0.028.
Values may be sent and summed in bfloat16 or wider, within the bound.
A program may use at most 128 MiB of HBM per device.

```python
import math
import jax
import jax.numpy as jnp
from jax import lax

D = 2048
FF = 5632
TOKENS = 1024
N_TP = 4


def draw_tokens(key, part):
    keys = jax.random.split(key, 7)
    column = jnp.arange(D, dtype=jnp.float32)
    place = (column + 0.5) * (2.0 / D) - 1.0
    flip = jnp.where(jax.random.uniform(keys[0], (TOKENS, 1), jnp.float32) < 0.5, -1.0, 1.0)
    tilt = flip * jax.random.uniform(keys[1], (TOKENS, 1), jnp.float32, 0.6, 1.0)
    rough = jnp.exp(jax.random.uniform(keys[2], (1, D), jnp.float32, -0.7, 0.7))
    dense = jnp.exp(tilt * place[None, :] * math.log(2.0)) * rough
    share = jnp.exp(jax.random.uniform(keys[3], (TOKENS, 1), jnp.float32, math.log(0.02), 0.0))
    center = jax.random.uniform(keys[4], (TOKENS, 1), jnp.float32, 0.0, 1.0) * D
    width = jnp.exp(jax.random.uniform(keys[5], (TOKENS, 1), jnp.float32, 0.0, math.log(3.0)))
    distance = jnp.abs(column[None, :] - center)
    distance = jnp.minimum(distance, D - distance)
    band = 4.0 * jnp.exp(-0.5 * jnp.square(distance / width))
    amplitude = share * dense + band
    values = jax.random.normal(keys[6], (TOKENS, D), jnp.float32) * amplitude
    return jnp.clip(values, -12.0, 12.0).astype(jnp.bfloat16)


def shard_levels(stream_key, dims, cuts, smallest, top_value):
    factor_of = 1.0
    for dim, parts in cuts:
        draws = jax.random.uniform(jax.random.fold_in(jax.random.fold_in(stream_key, 6), dim), (parts,), jnp.float32, smallest / len(cuts), top_value / len(cuts))
        factor_of = factor_of * jnp.repeat(jnp.exp(draws), dims[dim] // parts).reshape((-1,) + (1,) * (len(dims) - 1 - dim))
    return factor_of


def gaussian(stream_key, dims, spread, reach, shards=(), held_as=jnp.bfloat16):
    entries = jax.random.normal(stream_key, dims, jnp.float32) * spread
    if len(shards) > 0:
        entries = shard_levels(stream_key, dims, shards, -0.22, 0.18) * entries
    return jnp.clip(entries, min=-reach, max=reach).astype(held_as)


def setup_inputs(seed: int = 0, part: int = 0) -> dict:
    streams_of = jax.random.split(jax.random.key(seed), 16)
    own_keys = jax.random.split(jax.random.fold_in(streams_of[15], part), 16)
    return {
        "tokens": draw_tokens(jax.random.fold_in(jax.random.fold_in(streams_of[15], part), 71), part),
        "gain_first": jnp.clip(1.0 + 0.18 * jax.random.normal(streams_of[1], (D,), jnp.float32), 0.1, 1.9),
        "gate_first": gaussian(streams_of[2], (D, FF), D ** -0.5, 0.125, ((0, 4), (1, 4)), jnp.float32),
        "gate_scale_first": jnp.clip(jnp.exp(math.log(2.0) - 1.3862944 * jax.random.uniform(streams_of[3], (FF,), jnp.float32) ** shard_levels(streams_of[3], (FF,), ((0, 4),), -0.2, 0.2)), 0.5, 2.0),
        "up_first": gaussian(streams_of[4], (D, FF), D ** -0.5, 0.125, ((0, 4), (1, 4)), jnp.float32),
        "up_scale_first": jnp.clip(jnp.exp(math.log(2.0) - 1.3862944 * jax.random.uniform(streams_of[5], (FF,), jnp.float32) ** shard_levels(streams_of[5], (FF,), ((0, 4),), -0.2, 0.2)), 0.5, 2.0),
        "down_first": gaussian(streams_of[6], (FF, D), FF ** -0.5, 0.078125, ((0, 4), (1, 4)), jnp.float32),
        "down_scale_first": jnp.clip(jnp.exp(math.log(2.0) - 1.3862944 * jax.random.uniform(streams_of[7], (D,), jnp.float32) ** shard_levels(streams_of[7], (D,), ((0, 4),), -0.2, 0.2)), 0.5, 2.0),
        "gain_second": jnp.clip(1.0 + 0.18 * jax.random.normal(streams_of[8], (D,), jnp.float32), 0.1, 1.9),
        "gate_second": gaussian(streams_of[9], (D, FF), D ** -0.5, 0.125, ((0, 4), (1, 4)), jnp.float32),
        "gate_scale_second": jnp.clip(jnp.exp(math.log(2.0) - 1.3862944 * jax.random.uniform(streams_of[10], (FF,), jnp.float32) ** shard_levels(streams_of[10], (FF,), ((0, 4),), -0.2, 0.2)), 0.5, 2.0),
        "up_second": gaussian(streams_of[11], (D, FF), D ** -0.5, 0.125, ((0, 4), (1, 4)), jnp.float32),
        "up_scale_second": jnp.clip(jnp.exp(math.log(2.0) - 1.3862944 * jax.random.uniform(streams_of[12], (FF,), jnp.float32) ** shard_levels(streams_of[12], (FF,), ((0, 4),), -0.2, 0.2)), 0.5, 2.0),
        "down_second": gaussian(streams_of[13], (FF, D), FF ** -0.5, 0.078125, ((0, 4), (1, 4)), jnp.float32),
        "down_scale_second": jnp.clip(jnp.exp(math.log(2.0) - 1.3862944 * jax.random.uniform(streams_of[14], (D,), jnp.float32) ** shard_levels(streams_of[14], (D,), ((0, 4),), -0.2, 0.2)), 0.5, 2.0),
    }


epsilon = 1e-06

def down_total(hidden, down_bf16):
    block = FF // N_TP
    hidden_blocks = hidden.reshape(TOKENS, N_TP, block).transpose(1, 0, 2)
    weight_blocks = down_bf16.reshape(N_TP, block, D)

    def step(total, pair):
        partial_value = jnp.dot(pair[0], pair[1], preferred_element_type=jnp.float32).astype(jnp.bfloat16)
        partial_value = lax.optimization_barrier(partial_value)
        return (total + partial_value.astype(jnp.float32), None)
    total, _ = lax.scan(step, jnp.zeros((TOKENS, D), jnp.float32), (hidden_blocks, weight_blocks))
    return total

def block_apply(stream, gain, gate_w, gate_s, up_w, up_s, down_w, down_s):
    values = stream.astype(jnp.float32)
    mean_sq = lax.optimization_barrier(jnp.mean(values * values, axis=1, keepdims=True))
    normed = (values * lax.rsqrt(mean_sq + epsilon) * gain).astype(jnp.bfloat16)
    gate = jnp.dot(normed, gate_w.astype(jnp.bfloat16), preferred_element_type=jnp.float32) * gate_s
    up = jnp.dot(normed, up_w.astype(jnp.bfloat16), preferred_element_type=jnp.float32) * up_s
    hidden = (jax.nn.silu(gate) * up).astype(jnp.bfloat16)
    total = down_total(hidden, down_w.astype(jnp.bfloat16)) * down_s
    return (values + 0.5 * total).astype(jnp.bfloat16)

def reference(tokens, gain_first, gate_first, gate_scale_first, up_first, up_scale_first, down_first, down_scale_first, gain_second, gate_second, gate_scale_second, up_second, up_scale_second, down_second, down_scale_second):
    middle = block_apply(tokens, gain_first, gate_first, gate_scale_first, up_first, up_scale_first, down_first, down_scale_first)
    return block_apply(middle, gain_second, gate_second, gate_scale_second, up_second, up_scale_second, down_second, down_scale_second)
```

```python
import jax
import jax.numpy as jnp
from jax import lax
from jax.sharding import PartitionSpec as P

epsilon = 1e-06


def normalize(stream, gain):
    values = stream.astype(jnp.float32)
    totals = lax.psum(jnp.sum(values * values, axis=1), "tp")
    width = values.shape[1] * lax.axis_size("tp")
    normed = (values * lax.rsqrt(totals / width + epsilon)[:, None] * gain).astype(jnp.bfloat16)
    whole = lax.all_gather(normed, "tp", axis=1, tiled=True)
    return (values, whole)


def add_rows(whole, piece):
    return jnp.dot(whole, piece, preferred_element_type=jnp.float32)


def collect_gate_up(whole, gate_w, up_w):
    gate_bf = gate_w.astype(jnp.bfloat16)
    up_bf = up_w.astype(jnp.bfloat16)

    def add_one(piece):
        return add_rows(whole, piece)

    gate = add_one(lax.all_gather(gate_bf, "fs", axis=0, tiled=True))
    up = add_one(lax.all_gather(up_bf, "fs", axis=0, tiled=True))
    return (gate, up)


def collect_down(hidden, down_w):
    return jnp.dot(
        hidden,
        lax.all_gather(down_w.astype(jnp.bfloat16), "fs", axis=1, tiled=True),
        preferred_element_type=jnp.float32,
    )


def finish(values, gate, up, gate_s, up_s, down_s, down_fn):
    hidden = (jax.nn.silu(gate * gate_s) * (up * up_s)).astype(jnp.bfloat16)
    terms = down_fn(hidden)
    summed = lax.psum_scatter(
        terms.astype(jnp.bfloat16), "tp", scatter_dimension=1, tiled=True
    ).astype(jnp.float32)
    return (values + 0.5 * summed * down_s).astype(jnp.bfloat16)


def body_gather(
    tokens,
    gain_first,
    gate_first,
    gate_scale_first,
    up_first,
    up_scale_first,
    down_first,
    down_scale_first,
    gain_second,
    gate_second,
    gate_scale_second,
    up_second,
    up_scale_second,
    down_second,
    down_scale_second,
):
    values, whole = normalize(tokens, gain_first)
    gate, up = collect_gate_up(whole, gate_first, up_first)
    middle = finish(
        values,
        gate,
        up,
        gate_scale_first,
        up_scale_first,
        down_scale_first,
        lambda hidden: collect_down(hidden, down_first),
    )
    values, whole = normalize(middle, gain_second)
    gate, up = collect_gate_up(whole, gate_second, up_second)
    return finish(
        values,
        gate,
        up,
        gate_scale_second,
        up_scale_second,
        down_scale_second,
        lambda hidden: collect_down(hidden, down_second),
    )


def reshard_columns(weight):
    return lax.all_to_all(weight.astype(jnp.bfloat16), "fs", 1, 0, tiled=True)


def reshard_rows(weight):
    return lax.all_to_all(weight.astype(jnp.bfloat16), "fs", 0, 1, tiled=True)


def own_columns(scale):
    width = scale.shape[0] // lax.axis_size("fs")
    return lax.dynamic_slice_in_dim(scale, lax.axis_index("fs") * width, width)


def block(stream, gain, gate_w, gate_s, up_w, up_s, down_w, down_s):
    values, whole = normalize(stream, gain)
    every = lax.all_gather(whole, "fs", axis=0, tiled=True)
    gate = jnp.dot(every, gate_w, preferred_element_type=jnp.float32) * own_columns(gate_s)
    up = jnp.dot(every, up_w, preferred_element_type=jnp.float32) * own_columns(up_s)
    hidden = (jax.nn.silu(gate) * up).astype(jnp.bfloat16)
    terms = jnp.dot(hidden, down_w, preferred_element_type=jnp.float32).astype(jnp.bfloat16)
    mine = lax.psum_scatter(terms, "tp", scatter_dimension=1, tiled=True)
    summed = lax.psum_scatter(mine, "fs", scatter_dimension=0, tiled=True).astype(jnp.float32)
    return (values + 0.5 * summed * down_s).astype(jnp.bfloat16)


def body_reshard(
    tokens,
    gain_first,
    gate_first,
    gate_scale_first,
    up_first,
    up_scale_first,
    down_first,
    down_scale_first,
    gain_second,
    gate_second,
    gate_scale_second,
    up_second,
    up_scale_second,
    down_second,
    down_scale_second,
):
    weights = [
        (reshard_columns(gate), reshard_columns(up), reshard_rows(down))
        for gate, up, down in (
            (gate_first, up_first, down_first),
            (gate_second, up_second, down_second),
        )
    ]
    gate_w, up_w, down_w = weights[0]
    middle = block(
        tokens, gain_first, gate_w, gate_scale_first, up_w, up_scale_first, down_w, down_scale_first
    )
    gate_w, up_w, down_w = weights[1]
    return block(
        middle, gain_second, gate_w, gate_scale_second, up_w, up_scale_second, down_w, down_scale_second
    )


def solution(mesh):
    in_specs = (
        P(("grp", "fs"), "tp"),
        P("tp"),
        P("fs", "tp"),
        P("tp"),
        P("fs", "tp"),
        P("tp"),
        P("tp", "fs"),
        P("tp"),
        P("tp"),
        P("fs", "tp"),
        P("tp"),
        P("fs", "tp"),
        P("tp"),
        P("tp", "fs"),
        P("tp"),
    )
    out_specs = P(("grp", "fs"), "tp")
    def body(*args):
        width = args[2].shape[1] // lax.axis_size("fs")
        return (body_reshard if width >= 128 else body_gather)(*args)

    return jax.shard_map(body, mesh=mesh, in_specs=in_specs, out_specs=out_specs, check_vma=False)
```

```python
import functools

import jax
import jax.numpy as jnp
from jax import lax
from jax.experimental import pallas as pl
from jax.experimental.pallas import tpu as pltpu
from jax.sharding import PartitionSpec as P

MESH = pl.DeviceIdType.MESH

epsilon = 1e-06


def normalize(stream, gain):
    values = stream.astype(jnp.float32)
    totals = lax.psum(jnp.sum(values * values, axis=1), "tp")
    width = values.shape[1] * lax.axis_size("tp")
    normed = (values * lax.rsqrt(totals / width + epsilon)[:, None] * gain).astype(jnp.bfloat16)
    whole = lax.all_gather(normed, "tp", axis=1, tiled=True)
    return (values, whole)


def add_rows(whole, piece):
    return jnp.dot(whole, piece, preferred_element_type=jnp.float32)


def collect_gate_up(whole, gate_w, up_w):
    gate_bf = gate_w.astype(jnp.bfloat16)
    up_bf = up_w.astype(jnp.bfloat16)

    def add_one(piece):
        return add_rows(whole, piece)

    gate = add_one(lax.all_gather(gate_bf, "fs", axis=0, tiled=True))
    up = add_one(lax.all_gather(up_bf, "fs", axis=0, tiled=True))
    return (gate, up)


def collect_down(hidden, down_w):
    return jnp.dot(
        hidden,
        lax.all_gather(down_w.astype(jnp.bfloat16), "fs", axis=1, tiled=True),
        preferred_element_type=jnp.float32,
    )


def finish(values, gate, up, gate_s, up_s, down_s, down_fn):
    hidden = (jax.nn.silu(gate * gate_s) * (up * up_s)).astype(jnp.bfloat16)
    terms = down_fn(hidden)
    summed = lax.psum_scatter(
        terms.astype(jnp.bfloat16), "tp", scatter_dimension=1, tiled=True
    ).astype(jnp.float32)
    return (values + 0.5 * summed * down_s).astype(jnp.bfloat16)


def body_gather(
    tokens,
    gain_first,
    gate_first,
    gate_scale_first,
    up_first,
    up_scale_first,
    down_first,
    down_scale_first,
    gain_second,
    gate_second,
    gate_scale_second,
    up_second,
    up_scale_second,
    down_second,
    down_scale_second,
):
    values, whole = normalize(tokens, gain_first)
    gate, up = collect_gate_up(whole, gate_first, up_first)
    middle = finish(
        values,
        gate,
        up,
        gate_scale_first,
        up_scale_first,
        down_scale_first,
        lambda hidden: collect_down(hidden, down_first),
    )
    values, whole = normalize(middle, gain_second)
    gate, up = collect_gate_up(whole, gate_second, up_second)
    return finish(
        values,
        gate,
        up,
        gate_scale_second,
        up_scale_second,
        down_scale_second,
        lambda hidden: collect_down(hidden, down_second),
    )


def exchange_kernel(n_fs, *refs):
    z_send, z_recv, x_send, x_recv, own_sem = refs[-5:]
    count = (len(refs) - 5) // 3
    sources, results, held = (refs[i * count : (i + 1) * count] for i in range(3))
    grp, fs = lax.axis_index("grp"), lax.axis_index("fs")
    partner = {"grp": 1 - grp}
    peers = [lax.rem(fs + d, n_fs) for d in range(n_fs)]
    origins = [lax.rem(fs + n_fs - d, n_fs) for d in range(n_fs)]

    barrier = pltpu.get_barrier_semaphore()
    for d in range(1, n_fs):
        pl.semaphore_signal(barrier, inc=1, device_id={"fs": peers[d]}, device_id_type=MESH)
    pl.semaphore_signal(barrier, inc=1, device_id=partner, device_id_type=MESH)
    pl.semaphore_wait(barrier, n_fs)

    def my_half(ref):
        half = ref.shape[1] // 2
        return pl.ds(grp * half, half)

    def along_z(m, d):
        rows = my_half(sources[m])
        return pltpu.make_async_remote_copy(
            src_ref=sources[m].at[peers[d], rows],
            dst_ref=results[m].at[fs, rows],
            send_sem=z_send.at[m, d - 1],
            recv_sem=z_recv.at[m, d - 1],
            device_id={"fs": peers[d]},
            device_id_type=MESH,
        )

    def along_x(m, d):
        block = results[m].at[origins[d], my_half(results[m])]
        return pltpu.make_async_remote_copy(
            src_ref=block,
            dst_ref=block,
            send_sem=x_send.at[m, d - 1],
            recv_sem=x_recv.at[m, d - 1],
            device_id=partner,
            device_id_type=MESH,
        )

    order = [(m, d) for m in range(count) for d in range(1, n_fs)]
    for m, d in order:
        along_z(m, d).start()
    loads = [pltpu.make_async_copy(sources[m].at[fs], held[m], own_sem.at[m]) for m in range(count)]
    stores = [pltpu.make_async_copy(held[m], results[m].at[fs], own_sem.at[m]) for m in range(count)]
    for load in loads:
        load.start()
    for load, store in zip(loads, stores):
        load.wait()
        store.start()
    for m, d in order:
        along_z(m, d).wait_recv()
        along_x(m, d).start()
    for store in stores:
        store.wait()
    for m, d in order:
        along_z(m, d).wait_send()
        along_x(m, d).wait()


def column_chunks(weight):
    n = lax.axis_size("fs")
    parts = weight.astype(jnp.bfloat16).reshape(weight.shape[0], n, -1).transpose(1, 0, 2)
    return jnp.pad(parts, ((0, 0), (0, 0), (0, -parts.shape[2] % 128)))


def row_chunks(weight):
    return weight.astype(jnp.bfloat16).reshape(lax.axis_size("fs"), -1, weight.shape[1])


def exchange(which, arrays):
    n, count = lax.axis_size("fs"), len(arrays)
    any_spec = pl.BlockSpec(memory_space=pl.ANY)
    return pl.pallas_call(
        functools.partial(exchange_kernel, n),
        out_shape=[jax.ShapeDtypeStruct(a.shape, a.dtype) for a in arrays],
        in_specs=[any_spec] * count,
        out_specs=[any_spec] * count,
        scratch_shapes=[pltpu.VMEM(a.shape[1:], a.dtype) for a in arrays]
        + [pltpu.SemaphoreType.DMA((count, n - 1))] * 4
        + [pltpu.SemaphoreType.DMA((count,))],
        compiler_params=pltpu.CompilerParams(collective_id=which, has_side_effects=True),
        cost_estimate=pl.CostEstimate(
            flops=2 * 10**9 * count,
            bytes_accessed=4 * sum(a.size for a in arrays),
            transcendentals=0,
        ),
    )(*arrays)


def own_columns(scale):
    width = scale.shape[0] // lax.axis_size("fs")
    return lax.dynamic_slice_in_dim(scale, lax.axis_index("fs") * width, width)


def gather_kernel(n_fs, n_tp, block, out, held, own_sem, z_send, z_recv, y_send, y_recv, c_send, c_recv):
    fs, tp = lax.axis_index("fs"), lax.axis_index("tp")
    chips = n_tp // 2
    core = {"tp": tp + 1 - 2 * lax.rem(tp, 2)}
    peers = [lax.rem(fs + d, n_fs) for d in range(n_fs)]
    origins = [lax.rem(fs + n_fs - d, n_fs) for d in range(n_fs)]
    across = [lax.rem(tp + 2 * k, n_tp) for k in range(chips)]
    came_from = [lax.rem(tp + n_tp - 2 * k, n_tp) for k in range(chips)]

    barrier = pltpu.get_barrier_semaphore()
    greeted = [{"fs": p} for p in peers[1:]] + [{"tp": p} for p in across[1:]] + [core]
    for device in greeted:
        pl.semaphore_signal(barrier, inc=1, device_id=device, device_id_type=MESH)
    pl.semaphore_wait(barrier, len(greeted))

    def send(src, slot, sends, recvs, device):
        return pltpu.make_async_remote_copy(
            src_ref=src,
            dst_ref=out.at[slot],
            send_sem=sends,
            recv_sem=recvs,
            device_id=device,
            device_id_type=MESH,
        )

    def along_z(d):
        return send(block, (fs, tp), z_send.at[d], z_recv.at[d], {"fs": peers[d]})

    def along_y(d, k):
        src = block if d == 0 else out.at[origins[d], tp]
        return send(src, (origins[d], tp), y_send.at[d, k], y_recv.at[d, k], {"tp": across[k]})

    def to_core(d, k):
        slot = (origins[d], came_from[k])
        src = block if d == 0 and k == 0 else out.at[slot]
        return send(src, slot, c_send.at[d, k], c_recv.at[d, k], core)

    def pass_on(d):
        for k in range(1, chips):
            along_y(d, k).start()
        to_core(d, 0).start()

    def share(d):
        for k in range(1, chips):
            along_y(d, k).wait_recv()
            to_core(d, k).start()

    for d in range(1, n_fs):
        along_z(d).start()
    pass_on(0)
    load = pltpu.make_async_copy(block, held, own_sem)
    load.start()
    load.wait()
    store = pltpu.make_async_copy(held, out.at[fs, tp], own_sem)
    store.start()
    for d in range(1, n_fs):
        along_z(d).wait_recv()
        pass_on(d)
        share(d - 1)
    share(n_fs - 1)
    store.wait()
    for d in range(n_fs):
        if d > 0:
            along_z(d).wait_send()
        for k in range(chips):
            if k > 0:
                along_y(d, k).wait_send()
            to_core(d, k).wait()


def gather_tokens(which, stream):
    n_fs, n_tp = lax.axis_size("fs"), lax.axis_size("tp")
    any_spec = pl.BlockSpec(memory_space=pl.ANY)
    dma = pltpu.SemaphoreType.DMA
    whole = pl.pallas_call(
        functools.partial(gather_kernel, n_fs, n_tp),
        out_shape=jax.ShapeDtypeStruct((n_fs, n_tp, *stream.shape), stream.dtype),
        in_specs=[any_spec],
        out_specs=any_spec,
        scratch_shapes=[pltpu.VMEM(stream.shape, stream.dtype), dma(())]
        + [dma((n_fs,))] * 2
        + [dma((n_fs, n_tp // 2))] * 4,
        compiler_params=pltpu.CompilerParams(collective_id=which, has_side_effects=True),
        cost_estimate=pl.CostEstimate(
            flops=10**9, bytes_accessed=stream.size * 32, transcendentals=0
        ),
    )(stream)
    return whole.transpose(0, 2, 1, 3).reshape(n_fs * stream.shape[0], -1)


def scatter_kernel(
    n_fs, n_tp, terms, stream, scale, out, from_core, summed, from_y, total, from_z, acc,
    c_send, c_recv, y_send, y_recv, z_send, z_recv
):
    fs, tp = lax.axis_index("fs"), lax.axis_index("tp")
    chips = n_tp // 2
    flip = 1 - 2 * lax.rem(tp, 2)
    core = {"tp": tp + flip}
    peers = [lax.rem(fs + d, n_fs) for d in range(n_fs)]
    across = [lax.rem(tp + 2 * k, n_tp) for k in range(chips)]
    order = list(range(1, n_fs)) + [0]
    rows = stream.shape[0]
    step = 64

    barrier = pltpu.get_barrier_semaphore()
    greeted = [{"fs": p} for p in peers[1:]] + [{"tp": p} for p in across[1:]] + [core]
    for device in greeted:
        pl.semaphore_signal(barrier, inc=1, device_id=device, device_id_type=MESH)
    pl.semaphore_wait(barrier, len(greeted))

    def send(src, dst, sends, recvs, device):
        return pltpu.make_async_remote_copy(
            src_ref=src,
            dst_ref=dst,
            send_sem=sends,
            recv_sem=recvs,
            device_id=device,
            device_id_type=MESH,
        )

    def to_core(d, k):
        src = terms.at[across[k] + flip, peers[d]]
        return send(src, from_core.at[d, k], c_send.at[d, k], c_recv.at[d, k], core)

    def along_y(d, k):
        return send(
            summed.at[d, k], from_y.at[d, k], y_send.at[d, k], y_recv.at[d, k], {"tp": across[k]}
        )

    def along_z(d):
        return send(total.at[d], from_z.at[d], z_send.at[d], z_recv.at[d], {"fs": peers[d]})

    def combine(dst, parts):
        def one(i, carry):
            piece = pl.ds(i * step, step)
            value = parts[0][piece].astype(jnp.float32)
            for part in parts[1:]:
                value = value + part[piece].astype(jnp.float32)
            dst[piece] = value.astype(dst.dtype)
            return carry

        lax.fori_loop(0, rows // step, one, 0)

    for d in order:
        for k in reversed(range(chips)):
            to_core(d, k).start()
    for d in order:
        for k in reversed(range(chips)):
            to_core(d, k).wait_recv()
            if k > 0:
                combine(summed.at[d, k], [terms.at[across[k], peers[d]], from_core.at[d, k]])
                along_y(d, k).start()
    for d in order:
        for k in range(1, chips):
            along_y(d, k).wait_recv()
        parts = [terms.at[tp, peers[d]], from_core.at[d, 0]]
        parts = parts + [from_y.at[d, k] for k in range(1, chips)]
        combine(acc if d == 0 else total.at[d], parts)
        if d > 0:
            along_z(d).start()
    for d in range(1, n_fs):
        along_z(d).wait_recv()

    def finish_rows(i, carry):
        piece = pl.ds(i * step, step)
        value = acc[piece]
        for d in range(1, n_fs):
            value = value + from_z[d, piece].astype(jnp.float32)
        value = stream[piece].astype(jnp.float32) + 0.5 * value * scale[...]
        out[piece] = value.astype(out.dtype)
        return carry

    lax.fori_loop(0, rows // step, finish_rows, 0)
    for d in range(n_fs):
        if d > 0:
            along_z(d).wait_send()
        for k in range(chips):
            if k > 0:
                along_y(d, k).wait_send()
            to_core(d, k).wait_send()


def scatter_finish(which, terms, stream, scale):
    n_fs, n_tp = lax.axis_size("fs"), lax.axis_size("tp")
    chips = n_tp // 2
    tile = stream.shape
    vmem = pl.BlockSpec(memory_space=pltpu.VMEM)
    dma = pltpu.SemaphoreType.DMA
    half = jnp.bfloat16
    return pl.pallas_call(
        functools.partial(scatter_kernel, n_fs, n_tp),
        out_shape=jax.ShapeDtypeStruct(tile, half),
        in_specs=[vmem] * 3,
        out_specs=vmem,
        scratch_shapes=[
            pltpu.VMEM((n_fs, chips, *tile), half),
            pltpu.VMEM((n_fs, chips, *tile), half),
            pltpu.VMEM((n_fs, chips, *tile), half),
            pltpu.VMEM((n_fs, *tile), half),
            pltpu.VMEM((n_fs, *tile), half),
            pltpu.VMEM(tile, jnp.float32),
        ]
        + [dma((n_fs, chips))] * 4
        + [dma((n_fs,))] * 2,
        compiler_params=pltpu.CompilerParams(collective_id=which, has_side_effects=True),
        cost_estimate=pl.CostEstimate(
            flops=10**9, bytes_accessed=2 * terms.size, transcendentals=0
        ),
    )(terms.reshape(n_tp, n_fs, *tile), stream, scale[None, :])


def block(n, stream, gain, weights, gate_s, up_s, down_s, later):
    gate_w, up_w, down_w = weights
    every = gather_tokens(3 + n, stream).astype(jnp.float32)
    mean = jnp.mean(every * every, axis=1, keepdims=True)
    normed = (every * lax.rsqrt(mean + epsilon) * gain).astype(jnp.bfloat16)
    width = down_w.shape[1]

    def project(weight, scale):
        wide = jnp.dot(
            normed, weight.reshape(-1, weight.shape[2]), preferred_element_type=jnp.float32
        )
        return wide[:, :width] * own_columns(scale)

    hidden = (jax.nn.silu(project(gate_w, gate_s)) * project(up_w, up_s)).astype(jnp.bfloat16)
    terms = jnp.stack(
        [
            jnp.dot(hidden, w, preferred_element_type=jnp.float32).astype(jnp.bfloat16)
            for w in down_w
        ]
    )
    if not later:
        return scatter_finish(6, terms, stream, down_s), later
    terms, later = lax.optimization_barrier((terms, later))
    mine = lax.psum_scatter(terms, "tp", scatter_dimension=0, tiled=False)
    summed = lax.psum_scatter(mine, "fs", scatter_dimension=0, tiled=True)
    out = stream.astype(jnp.float32) + 0.5 * summed.astype(jnp.float32) * down_s
    return out.astype(jnp.bfloat16), later


def body_exchange(
    tokens,
    gain_first,
    gate_first,
    gate_scale_first,
    up_first,
    up_scale_first,
    down_first,
    down_scale_first,
    gain_second,
    gate_second,
    gate_scale_second,
    up_second,
    up_scale_second,
    down_second,
    down_scale_second,
):
    gains = lax.all_gather(jnp.stack([gain_first, gain_second]), "tp", axis=1, tiled=True)
    columns = exchange(0, [column_chunks(gate_first), column_chunks(up_first)])
    rows = exchange(1, [row_chunks(down_first)])
    later = ([column_chunks(gate_second), column_chunks(up_second)], [row_chunks(down_second)])
    middle, later = block(
        1,
        tokens,
        gains[0],
        (*columns, *rows),
        gate_scale_first,
        up_scale_first,
        down_scale_first,
        later,
    )
    columns = exchange(2, later[0])
    rows = exchange(3, later[1])
    return block(
        2,
        middle,
        gains[1],
        (*columns, *rows),
        gate_scale_second,
        up_scale_second,
        down_scale_second,
        (),
    )[0]


def solution(mesh):
    in_specs = (
        P(("grp", "fs"), "tp"),
        P("tp"),
        P("fs", "tp"),
        P("tp"),
        P("fs", "tp"),
        P("tp"),
        P("tp", "fs"),
        P("tp"),
        P("tp"),
        P("fs", "tp"),
        P("tp"),
        P("fs", "tp"),
        P("tp"),
        P("tp", "fs"),
        P("tp"),
    )
    out_specs = P(("grp", "fs"), "tp")

    def body(*args):
        n_fs, n_tp = lax.axis_size("fs"), lax.axis_size("tp")
        width = args[2].shape[1] // n_fs
        fits = width >= 128 and width % 32 == 0 and n_fs == n_tp and n_tp % 2 == 0 and lax.axis_size("grp") == 2
        fits = fits and args[0].shape[0] % 64 == 0
        return (body_exchange if fits else body_gather)(*args)

    return jax.shard_map(body, mesh=mesh, in_specs=in_specs, out_specs=out_specs, check_vma=False)
```
